32 devices in a mesh: sp: 4 (over y, x), tp: 8 (over z, core).
Axes of the slice: x: 2, y: 2, z: 4, core: 2. Of those that a mesh axis runs over, the one named last changes fastest.
Arguments:
- tokens: bfloat16 [2048, 2048], P(('sp', 'tp')), may hold values from -6 to 6
- query_vectors: bfloat16 [2048, 2048], P('sp', 'tp'), may hold values from -8 to 8
- key_vectors: bfloat16 [2048, 2048], P('sp', 'tp'), may hold values from -8 to 8
- value_vectors: bfloat16 [2048, 2048], P('sp', 'tp'), may hold values from -24 to 24
- cum_gate: float32 [2048, 32], P('sp', 'tp'), may hold values from -260 to 0, as said below
- out_weight: bfloat16 [2048, 2048], P('tp'), may hold values from -0.125 to 0.125
- norm_gain: float32 [2048], replicated, may hold values from 0.1 to 1.9
- gate_weight: bfloat16 [4, 2048, 7168], P('sp', None, 'tp'), may hold values from -0.125 to 0.125
- up_weight: bfloat16 [4, 2048, 7168], P('sp', None, 'tp'), may hold values from -0.125 to 0.125
- down_weight: bfloat16 [4, 7168, 2048], P('sp', 'tp'), may hold values from -0.0625 to 0.0625
- expert_ids: int32 [2048, 2], P(('sp', 'tp')), may hold values from 0 to 3, all different within a row; in each aligned block of 64 rows (0 to 63, 64 to 127, ...) at most 48 rows name the same one
- route_weights: float32 [2048, 2], P(('sp', 'tp')), may hold values from 0.2 to 1
Outputs:
- layer_output: bfloat16 [2048, 2048], P(('sp', 'tp'))
The draws below stay inside these ranges and needn't reach their ends.
Inputs may be any that keep to these rules, and one draw needn't show every extreme that they name: `cum_gate`: along the positions each head's values never rise. `expert_ids`: within the rows of one device no expert is named by more than 48 rows, and in some devices' rows one expert is named by exactly 48; a row names 2 different experts.
All inputs are finite; a program needn't handle non-finite values.
Results may differ from the reference program's by a relative error of at most 0.014.
Values may be sent and summed in bfloat16 or wider, within the bound.
A program may use at most 128 MiB of HBM per device.

```python
import math
import jax
import jax.numpy as jnp
import numpy as np
from jax import lax

D = 2048
HEAD_COUNT = 32
HEAD_DIM = 64
FFE = 7168
TOP = 2
TOK_SP = 512
EXPERTS = 4
TOKEN_COUNT = 2048
TOK_DEV = 64
CAP = 48


def paired_draw(key):
    parallel_flows = jax.random.split(jax.random.fold_in(key, 101), 2)
    width = HEAD_COUNT * HEAD_DIM
    query_part = jax.random.truncated_normal(parallel_flows[0], -6.0, 6.0, (TOKEN_COUNT, width), jnp.float32)
    key_part = jax.random.truncated_normal(parallel_flows[1], -6.0, 6.0, (TOKEN_COUNT, width), jnp.float32)
    return (query_part, key_part)


def draw_query_vectors(key, part):
    query_part, key_part = paired_draw(key)
    return query_part.astype(jnp.bfloat16)


def draw_key_vectors(key, part):
    query_part, key_part = paired_draw(key)
    return key_part.astype(jnp.bfloat16)


def draw_cum_gate(key, part):
    parallel_flows = jax.random.split(jax.random.fold_in(key, 202), 7)
    slow_cut = 8
    slow = jax.random.randint(parallel_flows[0], (HEAD_COUNT,), 0, 16) < slow_cut
    fast_rate = jnp.exp(jax.random.uniform(parallel_flows[1], (HEAD_COUNT,), jnp.float32, math.log(1.0 / 100.0), math.log(1.0 / 30.0)))
    slow_rate = jnp.exp(jax.random.uniform(parallel_flows[2], (HEAD_COUNT,), jnp.float32, 0.0, math.log(3.0))) / TOKEN_COUNT
    rate = jnp.where(slow, slow_rate, fast_rate)
    blocks = TOKEN_COUNT // TOK_SP
    step_levels = 2.0 ** jnp.linspace(-1.0, 1.0, blocks)
    step_levels = step_levels[jax.random.permutation(parallel_flows[3], blocks)]
    factor = jnp.repeat(step_levels, TOK_SP)
    rough = jax.random.uniform(parallel_flows[4], (TOKEN_COUNT, HEAD_COUNT), jnp.float32, 0.3, 1.7)
    descending_steps = rate[None, :] * factor[:, None] * rough
    spike_position = jax.random.randint(parallel_flows[5], (4,), 0, TOKEN_COUNT)
    spike_penalty = -jnp.log(1.0 - jax.random.uniform(parallel_flows[6], (4, HEAD_COUNT), jnp.float32, 0.2, 0.5))
    descending_steps = descending_steps.at[spike_position].add(spike_penalty)
    return jnp.cumsum(-descending_steps, axis=0)


def level_of(rng, shape, cuts, least, top_value):
    gain, own = 1.0, jax.random.fold_in(rng, 6)
    for dim, parts in cuts:
        draws = jnp.exp(jax.random.uniform(jax.random.fold_in(own, dim), (parts,), jnp.float32, least / len(cuts), top_value / len(cuts)))
        gain = gain * jnp.repeat(draws, shape[dim] // parts).reshape([-1 if axis == dim else 1 for axis in range(len(shape))])
    return gain


def routed_block(key, own, number, rows, count, top, limit, slope):
    ranking = jax.random.permutation(key, count)
    crowded, ordinary = portions_of(count, rows * top, limit, slope, True), portions_of(count, rows * top, limit, slope, False)
    places = jnp.arange(count)

    def named(tallies, offset_by):
        used = int((tallies > 0).sum())
        fixed = max(1, used // 4)
        passed = fixed + (places - fixed + offset_by * (used - fixed)) % max(1, count - fixed)
        return jnp.zeros((count,), jnp.int32).at[ranking[jnp.where(places < fixed, places, passed)]].set(jnp.asarray(tallies, jnp.int32))

    tallies = jnp.where(number % 4 == 0, named(crowded, number // 4), named(ordinary, number - number // 4 - 1))
    mixed = jax.random.permutation(jax.random.fold_in(own, 3), count)
    giver, receiver = mixed[0:count // 2 * 2:2], mixed[1:count // 2 * 2:2]
    slack = jnp.minimum(tallies[giver] - 1, limit - tallies[receiver]) // 2
    slack = jnp.where((giver == ranking[0]) | (receiver == ranking[0]) | (tallies[receiver] == 0), 0, jnp.maximum(slack, 0))
    passed = jax.random.randint(jax.random.fold_in(own, 4), (count // 2,), 0, 1 << 20) % (slack + 1)
    tallies = tallies.at[giver].add(-passed).at[receiver].add(passed)
    items = jnp.searchsorted(jnp.cumsum(tallies), jnp.arange(rows * top), side="right").astype(jnp.int32)
    listing = items.reshape(top, rows).T
    listing = listing[jax.random.permutation(jax.random.fold_in(own, 1), rows)]
    offset_by = jax.random.randint(jax.random.fold_in(own, 2), (rows, 1), 0, top)
    return jnp.take_along_axis(listing, (jnp.arange(top)[None, :] + offset_by) % top, axis=1)


def portions_of(count, total, most, skew, full):
    weights = [(1 << 20) // math.isqrt(grade ** skew) + 1 for grade in range(1, count + 1)]
    largest = most if full else min(most, max(-(-total // count), total * weights[0] // sum(weights)))
    least = 1 if total - largest >= count - 1 else 0
    given, surplus = [largest] + [least] * (count - 1), total - largest - least * (count - 1)
    while surplus > 0:
        free = [i for i in range(1, count) if given[i] < largest] or [i for i in range(1, count) if given[i] < most]
        mass, left = sum([weights[i] for i in free]), surplus
        for i in free:
            addition = min(most - given[i], max(1, left * weights[i] // mass), surplus)
            given[i] = given[i] + addition
            surplus = surplus - addition
    return np.array(given)


def scatter_about(key, extent, spread, reach, cuts=(), kind=jnp.bfloat16):
    loudness = level_of(key, extent, cuts, -0.22, 0.18) if cuts else 1.0
    entries = jax.random.normal(key, extent, jnp.float32) * spread * loudness
    return jnp.minimum(jnp.maximum(entries, -reach), reach).astype(kind)


def setup_inputs(seed: int = 0) -> dict:
    key_list = jax.random.split(jax.random.key(seed), 13)
    tokens = scatter_about(key_list[0], (TOKEN_COUNT, D), 1.0, 6.0, ((0, 32),))
    query_vectors = draw_query_vectors(jax.random.fold_in(key_list[12], 71), 0)
    key_vectors = draw_key_vectors(jax.random.fold_in(key_list[12], 71), 0)
    value_vectors = scatter_about(key_list[3], (TOKEN_COUNT, HEAD_COUNT * HEAD_DIM), 4.0, 24.0, ((0, 4), (1, 8)))
    cum_gate = draw_cum_gate(jax.random.fold_in(key_list[12], 71), 0)
    out_weight = scatter_about(key_list[5], (HEAD_COUNT * HEAD_DIM, D), (HEAD_COUNT * HEAD_DIM) ** -0.5, 0.125, ((0, 8),))
    norm_gain = jnp.clip(1.0 + 0.18 * jax.random.normal(key_list[6], (D,), jnp.float32), 0.1, 1.9)
    gate_weight = scatter_about(key_list[7], (EXPERTS, D, FFE), D ** -0.5, 0.125, ((0, 4), (2, 8)))
    up_weight = scatter_about(key_list[8], (EXPERTS, D, FFE), D ** -0.5, 0.125, ((0, 4), (2, 8)))
    down_weight = scatter_about(key_list[9], (EXPERTS, FFE, D), FFE ** -0.5, 0.0625, ((0, 4), (1, 8)))
    expert_ids_keys = jax.random.split(jax.random.fold_in(key_list[10], 1), TOKEN_COUNT // TOK_DEV)
    expert_ids_turns = jax.random.permutation(jax.random.fold_in(key_list[10], 3), TOKEN_COUNT // TOK_DEV)
    expert_ids = jax.vmap(lambda own, number: routed_block(jax.random.fold_in(key_list[10], 2), own, number, TOK_DEV, EXPERTS, TOP, CAP, 1))(expert_ids_keys, expert_ids_turns).reshape((TOKEN_COUNT, TOP))
    route_weights = jnp.clip(0.2 + 0.8 * jax.random.uniform(key_list[11], (TOKEN_COUNT, TOP), jnp.float32) ** level_of(key_list[11], (TOKEN_COUNT, TOP), ((0, 32),), -0.2, 0.2), 0.2, 1.0)
    return {"tokens": tokens, "query_vectors": query_vectors, "key_vectors": key_vectors, "value_vectors": value_vectors, "cum_gate": cum_gate, "out_weight": out_weight, "norm_gain": norm_gain, "gate_weight": gate_weight, "up_weight": up_weight, "down_weight": down_weight, "expert_ids": expert_ids, "route_weights": route_weights}


def reference(tokens, query_vectors, key_vectors, value_vectors, cum_gate, out_weight, norm_gain, gate_weight, up_weight, down_weight, expert_ids, route_weights):
    score_scale = HEAD_DIM ** (-0.5)
    query_block = math.gcd(TOKEN_COUNT, 512)
    block_count = TOKEN_COUNT // query_block
    all_positions = jnp.arange(TOKEN_COUNT, dtype=jnp.int32)

    def head_output(head_index):
        column = (head_index * HEAD_DIM).astype(jnp.int32)
        query_head = lax.dynamic_slice_in_dim(query_vectors, column, HEAD_DIM, 1)
        key_head = lax.dynamic_slice_in_dim(key_vectors, column, HEAD_DIM, 1)
        value_head = lax.dynamic_slice_in_dim(value_vectors, column, HEAD_DIM, 1)
        gate_head = lax.dynamic_slice_in_dim(cum_gate, head_index.astype(jnp.int32), 1, 1)[:, 0]

        def block_output(block_index):
            first_row = (block_index * query_block).astype(jnp.int32)
            query_rows = lax.dynamic_slice_in_dim(query_head, first_row, query_block, 0)
            gate_rows = lax.dynamic_slice_in_dim(gate_head, first_row, query_block, 0)
            scores = jnp.dot(query_rows, key_head.T, preferred_element_type=jnp.float32) * score_scale
            scores = scores + gate_rows[:, None] - gate_head[None, :]
            query_pos = first_row + jnp.arange(query_block, dtype=jnp.int32)
            visible = all_positions[None, :] <= query_pos[:, None]
            scores = jnp.where(visible, scores, -jnp.inf)
            peak = lax.optimization_barrier(jnp.max(scores, axis=1, keepdims=True))
            exponent = jnp.exp(scores - peak)
            denominator = lax.optimization_barrier(jnp.sum(exponent, axis=1))
            probs = exponent.astype(jnp.bfloat16)
            summed = jnp.dot(probs, value_head, preferred_element_type=jnp.float32)
            return (summed / denominator[:, None]).astype(jnp.bfloat16)
        blocks = lax.map(block_output, jnp.arange(block_count, dtype=jnp.int32))
        return blocks.reshape(TOKEN_COUNT, HEAD_DIM)
    per_head = lax.map(head_output, jnp.arange(HEAD_COUNT, dtype=jnp.int32))
    attended = per_head.transpose(1, 0, 2).reshape(TOKEN_COUNT, HEAD_COUNT * HEAD_DIM)
    projected = jnp.dot(attended, out_weight, preferred_element_type=jnp.float32)
    stream = (tokens.astype(jnp.float32) + projected).astype(jnp.bfloat16)
    stream_wide = stream.astype(jnp.float32)
    inverse = lax.rsqrt(lax.optimization_barrier(jnp.mean(stream_wide * stream_wide, axis=1, keepdims=True)) + 1e-05)
    normed = (stream_wide * inverse * norm_gain[None, :]).astype(jnp.bfloat16)
    route_count = TOKEN_COUNT * TOP
    most_rows = TOKEN_COUNT // TOK_DEV * CAP
    flat_ids = expert_ids.reshape(-1)
    route_order = jnp.arange(route_count, dtype=jnp.int32)

    def expert_pass(routed_out, expert_index):
        sort_keys = jnp.where(flat_ids == expert_index, 0, 1) * route_count + route_order
        chosen = jnp.argsort(sort_keys)[:most_rows].astype(jnp.int32)
        valid = flat_ids[chosen] == expert_index
        rows_in = normed[chosen // TOP]
        gate_value = jnp.dot(rows_in, gate_weight[expert_index], preferred_element_type=jnp.float32)
        up_value = jnp.dot(rows_in, up_weight[expert_index], preferred_element_type=jnp.float32)
        hidden = (jax.nn.silu(gate_value) * up_value).astype(jnp.bfloat16)
        expert_out = jnp.dot(hidden, down_weight[expert_index], preferred_element_type=jnp.float32).astype(jnp.bfloat16)
        current = routed_out[chosen]
        routed_out = routed_out.at[chosen].set(jnp.where(valid[:, None], expert_out, current))
        return (routed_out, None)
    routed_out, _ = lax.scan(expert_pass, jnp.zeros((route_count, D), jnp.bfloat16), jnp.arange(EXPERTS, dtype=jnp.int32))
    routed = routed_out.reshape(TOKEN_COUNT, TOP, D).astype(jnp.float32)
    mixture = lax.optimization_barrier(jnp.sum(routed * route_weights[:, :, None], axis=1))
    return (stream_wide + mixture).astype(jnp.bfloat16)
```

```python
import functools
import math

import jax
import jax.numpy as jnp
from jax import lax
from jax.experimental import pallas as pl
from jax.experimental.pallas import tpu as pltpu
from jax.sharding import PartitionSpec as P

MESH = pl.DeviceIdType.MESH
VMEM_LIMIT = 60 * 1024 * 1024
F32 = jnp.float32
BF16 = jnp.bfloat16


def rcopy(src, dst, ssem, rsem, where):
    return pltpu.make_async_remote_copy(
        src_ref=src, dst_ref=dst, send_sem=ssem, recv_sem=rsem, device_id=where, device_id_type=MESH
    )


def vmem_specs(count):
    return [pl.BlockSpec(memory_space=pltpu.VMEM)] * count


def layer_kernel(
    sp, zn, heads, cap,
    q, k, v, g, tok, gain, ids, rw, w_in, wg_in, wu_in, wd_in, out,
    ka, va, ga, att, attp, top_s, sum_s, acc_s, wo, pf, sup, sdn, rup, rdn, ng,
    info, code, combs, wg, wu, wd, db, rows, hid, y, pr, cs, eb, mb, rr,
    ks, krs, ws, wxs, hs, as_, ars, us, urs, ns, nrs, ds_, drs, fs, frs, ps, prs, es, ers, ms, mrs,
):
    s, t = lax.axis_index("sp"), lax.axis_index("tp")
    z, c = lax.div(t, 2), lax.rem(t, 2)
    partner = t + 1 - 2 * c
    T, D = tok.shape
    seg, width = q.shape
    hd = width // heads
    loads = [
        pltpu.make_async_copy(a, b, ws.at[n])
        for n, (a, b) in enumerate(
            ((w_in, wo.at[0]), (wg_in.at[0], wg), (wu_in.at[0], wu), (wd_in.at[0], wd))
        )
    ]
    for load in loads:
        load.start()

    def at_z(zz):
        return {"tp": 2 * lax.rem(zz + zn, zn) + c}

    def peer(d):
        return lax.rem(s + d, sp)

    def behind(d):
        return lax.rem(s + sp - d, sp)

    barrier = pltpu.get_barrier_semaphore()
    pl.semaphore_signal(barrier, inc=1, device_id={"tp": partner}, device_id_type=MESH)
    for i in range(1, zn):
        pl.semaphore_signal(barrier, inc=1, device_id=at_z(z + i), device_id_type=MESH)
    for d in range(1, sp):
        pl.semaphore_signal(barrier, inc=1, device_id={"sp": peer(d)}, device_id_type=MESH)
    pl.semaphore_wait(barrier, 1 + (zn - 1) + (sp - 1))

    pairs = ((k, ka), (v, va), (g, ga))

    def share(n, d):
        src, dst = pairs[n]
        return rcopy(src, dst.at[d], ks.at[n, d], krs.at[n, d], {"sp": peer(d)})

    for d in range(1, sp):

        @pl.when(s + d < sp)
        def _():
            for n in range(3):
                share(n, d).start()

    weights = rcopy(w_in, wo.at[1], wxs.at[0], wxs.at[1], {"tp": partner})
    weights.start()

    many = info.shape[2]
    here = lax.broadcasted_iota(jnp.int32, (many, T), 0)
    hit = jnp.zeros((many, T), F32)
    wt = jnp.zeros((many, T), F32)
    for r in range(ids.shape[0]):
        same = ids[r : r + 1, :] == here
        hit = hit + jnp.where(same, 1.0, 0.0)
        wt = wt + jnp.where(same, rw[r : r + 1, :], 0.0)
    before = lax.broadcasted_iota(jnp.int32, (T, T), 0) < lax.broadcasted_iota(jnp.int32, (T, T), 1)
    rank = jnp.dot(
        hit.astype(BF16), jnp.where(before, 1.0, 0.0).astype(BF16), preferred_element_type=F32
    )
    info[z, 0] = jnp.where(hit > 0.5, rank, -1.0)
    info[z, 1] = wt

    def aux(i, origin):
        return rcopy(info.at[origin], info.at[origin], as_.at[i], ars.at[i], at_z(z + i))

    for i in range(1, zn):
        aux(i, z).start()

    tile = math.gcd(seg, 256)
    log2e = 1.4426950408889634
    coef = hd ** (-0.5) * log2e
    units = [(h, i) for h in range(heads) for i in range(seg // tile)]

    def scores(h, i, kb, gb):
        qt = q[i * tile : (i + 1) * tile, h * hd : (h + 1) * hd]
        return (
            lax.dot_general(qt, kb, (((1,), (1,)), ((), ())), preferred_element_type=F32) * coef
            - gb * log2e
        )

    for h, i in units:
        cols = slice(h * hd, (h + 1) * hd)
        seen = (i + 1) * tile
        sc = scores(h, i, k[0:seen, cols], g[h : h + 1, 0:seen])
        row = lax.broadcasted_iota(jnp.int32, sc.shape, 0) + i * tile
        col = lax.broadcasted_iota(jnp.int32, sc.shape, 1)
        sc = jnp.where(col <= row, sc, -1e30)
        peak = jnp.max(sc, axis=1, keepdims=True)
        ex = jnp.exp2(sc - peak)
        at = slice(i * tile, seen)
        top_s[h, at] = peak
        sum_s[h, at] = jnp.sum(ex, axis=1, keepdims=True)
        acc_s[h, at] = jnp.dot(ex.astype(BF16), v[0:seen, cols], preferred_element_type=F32)

    def step(d, _):
        for n in range(3):
            share(n, d).wait_recv()
        for h, i in units:
            cols = slice(h * hd, (h + 1) * hd)
            at = slice(i * tile, (i + 1) * tile)
            sc = scores(h, i, ka[d, :, cols], ga[d, h : h + 1, :])
            peak = top_s[h, at]
            new = jnp.maximum(peak, jnp.max(sc, axis=1, keepdims=True))
            ex = jnp.exp2(sc - new)
            fix = jnp.exp2(peak - new)
            top_s[h, at] = new
            sum_s[h, at] = sum_s[h, at] * fix + jnp.sum(ex, axis=1, keepdims=True)
            acc_s[h, at] = acc_s[h, at] * fix + jnp.dot(
                ex.astype(BF16), va[d, :, cols], preferred_element_type=F32
            )
        return 0

    lax.fori_loop(1, s + 1, step, 0)
    for h, i in units:
        for b in range(i * tile // T, (i + 1) * tile // T):
            at = slice(b * T, (b + 1) * T)
            att[b % 2, b // 2, :, h * hd : (h + 1) * hd] = (acc_s[h, at] / sum_s[h, at]).astype(BF16)
    heads_swap = rcopy(att.at[1 - c], attp, hs.at[0], hs.at[1], {"tp": partner})
    heads_swap.start()
    loads[0].wait()
    weights.wait_recv()
    heads_swap.wait_recv()

    halves = 2
    part = D // halves
    chunk = math.gcd(part, 512)
    mine = att[c].reshape(zn * T, width)
    other = attp[...].reshape(zn * T, width)

    def hop(up, dest, h):
        cut = slice(h * part, (h + 1) * part)
        src, dst = (sup, rup) if up else (sdn, rdn)
        return rcopy(
            src.at[dest, :, cut], dst.at[dest, :, cut], us.at[up, dest, h], urs.at[up, dest, h],
            at_z(z + 1 if up else z - 1),
        )

    def project(h):
        for n in range(part // chunk):
            cut = slice(h * part + n * chunk, h * part + (n + 1) * chunk)
            got = jnp.dot(mine, wo[0, :, cut], preferred_element_type=F32) + jnp.dot(
                other, wo[1, :, cut], preferred_element_type=F32
            )
            pf[:, :, cut] = got.reshape(zn, T, chunk)

    def push(kk, h):
        cut = slice(h * part, (h + 1) * part)
        for up in (1, 0):
            dest = zn - 1 - kk if up else kk
            going = z < dest if up else z > dest
            first = z == 0 if up else z == zn - 1
            inner = z > 0 if up else z < zn - 1
            src, dst = (sup, rup) if up else (sdn, rdn)

            @pl.when(jnp.logical_and(going, first))
            def _():
                src[dest, :, cut] = pf[dest, :, cut].astype(BF16)
                hop(up, dest, h).start()

            @pl.when(jnp.logical_and(going, inner))
            def _():
                hop(up, dest, h).wait_recv()
                src[dest, :, cut] = (pf[dest, :, cut] + dst[dest, :, cut].astype(F32)).astype(BF16)
                hop(up, dest, h).start()

    for h in range(halves):
        project(h)
        if h == 0:
            pass
    for kk in range(zn - 1):
        for h in range(halves):
            push(kk, h)
    for h in range(halves):
        cut = slice(h * part, (h + 1) * part)

        @pl.when(z > 0)
        def _():
            hop(1, z, h).wait_recv()
            pf[z, :, cut] = pf[z, :, cut] + rup[z, :, cut].astype(F32)

        @pl.when(z < zn - 1)
        def _():
            hop(0, z, h).wait_recv()
            pf[z, :, cut] = pf[z, :, cut] + rdn[z, :, cut].astype(F32)

    st = (tok[...].astype(F32) + pf[z]).astype(BF16)
    out[...] = st
    wide = st.astype(F32)
    inverse = lax.rsqrt(jnp.mean(wide * wide, axis=1, keepdims=True) + 1e-05)
    ng[z] = (wide * inverse * gain[...]).astype(BF16)

    high = lax.div(2 * z, zn)
    low_z = z + high * (zn - 1 - 2 * z)

    def origin(j):
        if j == 0:
            return z
        a = (j + 1) // 2
        near = lax.div(zn + low_z - a, zn)
        o = near * (low_z + (a if j % 2 == 0 else -a)) + (1 - near) * j
        return o + high * (zn - 1 - 2 * o)

    def along(o):
        up = lax.div(zn + z - o - 1, zn)
        far = up * (z - o) + (1 - up) * (o - z)
        return up, far

    def carry(o, up, far):
        ref = ng.at[o]
        return rcopy(ref, ref, ns.at[up, far], nrs.at[up, far], at_z(z + 2 * up - 1))

    def arrived(o, up, far):
        ref = ng.at[o]
        return rcopy(ref, ref, ns.at[up, far], nrs.at[up, far - 1], at_z(z))

    def onward(o, up, far, act):
        goes = z + 2 * up - 1

        @pl.when(jnp.logical_and(goes >= 0, goes < zn))
        def _():
            act(carry(o, up, far))

    def own_block(act):
        @pl.when(z < zn - 1)
        def _():
            act(carry(z, 1, 0))

        @pl.when(z > 0)
        def _():
            act(carry(z, 0, 0))

    own_block(lambda cp: cp.start())

    def route(j, d):
        return rcopy(
            db.at[j, peer(d)], rows.at[j, s, c], ds_.at[j, d], drs.at[j, d], {"sp": peer(d)}
        )

    def routed(j, d):
        return rcopy(
            db.at[j, peer(d)], rows.at[j, behind(d), c], ds_.at[j, d], drs.at[j, d], {"sp": peer(d)}
        )

    def forward(j, d):
        ref = rows.at[j, behind(d), c]
        return rcopy(ref, ref, fs.at[j, d], frs.at[j, d], {"tp": partner})

    def forwarded(j, d):
        ref = rows.at[j, behind(d), 1 - c]
        return rcopy(ref, ref, fs.at[j, d], frs.at[j, d], {"tp": partner})

    def swap_out(j, d):
        return rcopy(y.at[j, peer(d), 1 - c], pr.at[j, d], ps.at[j, d], prs.at[j, d], {"tp": partner})

    def back(j, d, slot):
        return rcopy(cs.at[j, d], eb.at[j, slot], es.at[j, d], ers.at[j, d], {"sp": peer(d)})

    def reduce_out(j):
        return rcopy(mb.at[j], rr.at[z], ms.at[j], mrs.at[z], at_z(origin(j)))

    def reduced(i):
        zz = lax.rem(z + i, zn)
        return rcopy(mb.at[0], rr.at[zz], ms.at[0], mrs.at[zz], at_z(z))

    def dispatch(j):
        o = origin(j)
        if j > 0:
            up, far = along(o)
            arrived(o, up, far).wait_recv()
            onward(o, up, far, lambda cp: cp.start())
            aux(lax.rem(z - o + zn, zn), o).wait_recv()
        spots = lax.broadcasted_iota(jnp.int32, (cap, T), 0).astype(F32)
        for e in range(sp):
            code[e * cap : (e + 1) * cap] = jnp.where(info[o, 0, e : e + 1, :] == spots, 1.0, 0.0)
        moved = jnp.dot(code[...].astype(BF16), ng[o], preferred_element_type=F32)
        for e in range(sp):
            db[j, e] = moved[e * cap : (e + 1) * cap].astype(BF16)
        for d in range(1, sp):
            route(j, d).start()
        rows[j, s, c] = db[j, s]
        forward(j, 0).start()
        for e in range(sp):
            code[e * cap : (e + 1) * cap] = jnp.where(
                info[o, 0, e : e + 1, :] == spots, jnp.broadcast_to(info[o, 1, e : e + 1, :], (cap, T)), 0.0
            )
        given = code[...]
        coarse = given.astype(BF16)
        combs[j, 0] = coarse
        combs[j, 1] = (given - coarse.astype(F32)).astype(BF16)

    def pass_on(j):
        def arrive(d, _):
            routed(j, d).wait_recv()
            forward(j, d).start()
            return 0

        lax.fori_loop(1, sp, arrive, 0)

    def each(count, body):
        if count * rows.shape[1] <= 64:
            for n in range(count):
                body(n)
        else:
            lax.fori_loop(0, count, lambda n, _: (body(n), 0)[1], 0)

    def expert(j):
        def landed(d, _):
            forwarded(j, d).wait_recv()
            return 0

        lax.fori_loop(0, sp, landed, 0)
        x = rows.at[j]
        many = sp * 2 * cap
        units = wg.shape[1]
        step = 256

        def into(start, size):
            cut = pl.ds(start, size)
            xv = x[...].reshape(many, D)
            gate = jnp.dot(xv, wg[:, cut], preferred_element_type=F32)
            up = jnp.dot(xv, wu[:, cut], preferred_element_type=F32)
            hid[:, cut] = (gate / (1.0 + jnp.exp(-gate)) * up).astype(BF16)

        each(units // step, lambda n: into(pl.multiple_of(n * step, step), step))
        if units % step:
            into(units - units % step, units % step)
        chunk = math.gcd(D, 512)

        def down(n):
            cut = pl.ds(pl.multiple_of(n * chunk, chunk), chunk)
            got = jnp.dot(hid[...], wd[:, cut], preferred_element_type=F32).astype(BF16)
            y[j, :, :, :, cut] = got.reshape(sp, 2, cap, chunk)

        each(D // chunk, down)
        for d in list(range(1, sp)) + [0]:
            swap_out(j, d).start()

    def give_back(j):
        def both(d):
            swap_out(j, d).wait_recv()
            return (y[j, peer(d), c].astype(F32) + pr[j, d].astype(F32)).astype(BF16)

        def send(d, _):
            cs[j, d] = both(d)
            back(j, d, s).start()
            return 0

        lax.fori_loop(1, sp, send, 0)
        eb[j, s] = both(0)

    def mix(j):
        for d in range(1, sp):
            back(j, d, behind(d)).wait_recv()
        ev = eb[j].reshape(sp * cap, D)
        dims = (((0,), (0,)), ((), ()))
        return lax.dot_general(combs[j, 0], ev, dims, preferred_element_type=F32) + lax.dot_general(
            combs[j, 1], ev, dims, preferred_element_type=F32
        )

    dispatch(0)
    if zn > 1:
        dispatch(1)
    for load in loads[1:]:
        load.wait()
    for j in range(zn):
        pass_on(j)
        if j + 2 < zn:
            dispatch(j + 2)
        expert(j)
        if j >= 2:
            give_back(j - 1)
    if zn > 1:
        give_back(zn - 1)
    give_back(0)
    for j in range(1, zn):
        mb[j] = mix(j).astype(BF16)
        reduce_out(j).start()
    total = out[...].astype(F32) + mix(0)
    for i in range(1, zn):
        reduced(i).wait_recv()
        total = total + rr[lax.rem(z + i, zn)].astype(F32)
    out[...] = total.astype(BF16)

    for d in range(1, sp):

        @pl.when(s + d < sp)
        def _():
            for n in range(3):
                share(n, d).wait_send()

    weights.wait_send()
    heads_swap.wait_send()
    own_block(lambda cp: cp.wait_send())
    for kk in range(zn - 1):
        for h in range(halves):
            for up in (1, 0):
                dest = zn - 1 - kk if up else kk

                @pl.when(z < dest if up else z > dest)
                def _():
                    hop(up, dest, h).wait_send()

    for j in range(zn):
        if j > 0:
            aux(j, z).wait_send()
            o = origin(j)
            onward(o, *along(o), lambda cp: cp.wait_send())
            reduce_out(j).wait_send()

        def drain(d, _):
            forward(j, d).wait_send()
            swap_out(j, d).wait_send()
            return 0

        lax.fori_loop(0, sp, drain, 0)
        for d in range(1, sp):
            route(j, d).wait_send()
            back(j, d, s).wait_send()


def shards(
    tokens,
    query_vectors,
    key_vectors,
    value_vectors,
    cum_gate,
    out_weight,
    norm_gain,
    gate_weight,
    up_weight,
    down_weight,
    expert_ids,
    route_weights,
):
    sp = lax.axis_size("sp")
    tp = lax.axis_size("tp")
    zn = tp // 2
    seg, width = query_vectors.shape
    heads = cum_gate.shape[1]
    T, D = tokens.shape
    dma = pltpu.SemaphoreType.DMA

    n_experts = gate_weight.shape[0] * sp
    top = expert_ids.shape[1]
    cap = max(2, 3 * T * top // (2 * n_experts))
    cap = -(-cap // 8) * 8
    slots = n_experts * cap
    kinds = -(-n_experts // 8) * 8
    fh = gate_weight.shape[2]

    def vm(*shape, kind=BF16):
        return pltpu.VMEM(shape, kind)

    return pl.pallas_call(
        functools.partial(layer_kernel, sp, zn, heads, cap),
        out_shape=jax.ShapeDtypeStruct((T, D), BF16),
        in_specs=vmem_specs(8) + [pl.BlockSpec(memory_space=pl.ANY)] * 4,
        out_specs=vmem_specs(1)[0],
        scratch_shapes=[
            vm(sp, seg, width), vm(sp, seg, width), vm(sp, heads, seg, kind=F32),
            vm(2, zn, T, width), vm(zn, T, width),
            vm(heads, seg, 1, kind=F32), vm(heads, seg, 1, kind=F32),
            vm(heads, seg, width // heads, kind=F32),
            vm(2, width, D), vm(zn, T, D, kind=F32),
            vm(zn, T, D), vm(zn, T, D), vm(zn, T, D), vm(zn, T, D), vm(zn, T, D),
            vm(zn, 2, kinds, T, kind=F32), vm(slots, T, kind=F32), vm(zn, 2, slots, T),
            vm(D, fh), vm(D, fh), vm(fh, D),
            vm(zn, sp, cap, D),
            vm(zn, sp, 2, cap, D),
            vm(sp * 2 * cap, fh),
            vm(zn, sp, 2, cap, D),
            vm(zn, sp, cap, D), vm(zn, sp, cap, D), vm(zn, sp, cap, D),
            vm(zn, T, D), vm(zn, T, D),
            dma((3, sp)), dma((3, sp)),
            dma((4,)), dma((2,)), dma((2,)),
            dma((zn,)), dma((zn,)),
            dma((2, zn, 2)), dma((2, zn, 2)),
            dma((2, zn)), dma((2, zn)),
            dma((zn, sp)), dma((zn, sp)),
            dma((zn, sp)), dma((zn, sp)),
            dma((zn, sp)), dma((zn, sp)),
            dma((zn, sp)), dma((zn, sp)),
            dma((zn,)), dma((zn,)),
        ],
        compiler_params=pltpu.CompilerParams(
            collective_id=0, has_side_effects=True, vmem_limit_bytes=VMEM_LIMIT
        ),
        name="layer",
    )(
        query_vectors, key_vectors, value_vectors, cum_gate.T, tokens, norm_gain[None, :],
        expert_ids.T, route_weights.T, out_weight, gate_weight, up_weight, down_weight,
    )


def solution(mesh):
    in_specs = (
        P(("sp", "tp"), None),
        P("sp", "tp"),
        P("sp", "tp"),
        P("sp", "tp"),
        P("sp", "tp"),
        P("tp", None),
        P(),
        P("sp", None, "tp"),
        P("sp", None, "tp"),
        P("sp", "tp", None),
        P(("sp", "tp"), None),
        P(("sp", "tp"), None),
    )
    out_specs = P(("sp", "tp"), None)
    return jax.shard_map(shards, mesh=mesh, in_specs=in_specs, out_specs=out_specs, check_vma=False)
```

```python
import functools
import math

import jax
import jax.numpy as jnp
from jax import lax
from jax.experimental import pallas as pl
from jax.experimental.pallas import tpu as pltpu
from jax.sharding import PartitionSpec as P

MESH = pl.DeviceIdType.MESH
VMEM_LIMIT = 60 * 1024 * 1024
F32 = jnp.float32
BF16 = jnp.bfloat16


def rcopy(src, dst, ssem, rsem, where):
    return pltpu.make_async_remote_copy(
        src_ref=src, dst_ref=dst, send_sem=ssem, recv_sem=rsem, device_id=where, device_id_type=MESH
    )


def vmem_specs(count):
    return [pl.BlockSpec(memory_space=pltpu.VMEM)] * count


def layer_kernel(
    sp, zn, heads, cap,
    q, k, v, g, tok, gain, ids, rw, w_in, wg_in, wu_in, wd_in, out,
    ka, va, ga, att, attp, top_s, sum_s, acc_s, wo, pf, sup, sdn, rup, rdn, ng,
    info, code, combs, wg, wu, wd, db, rows, hid, y, pr, cs, eb, mb, rr,
    ks, krs, kx, gs, ws, wxs, hs, as_, ars, us, urs, ns, nrs, ds_, drs, fs, frs, ps, prs, es, ers, ms, mrs,
):
    s, t = lax.axis_index("sp"), lax.axis_index("tp")
    z, c = lax.div(t, 2), lax.rem(t, 2)
    partner = t + 1 - 2 * c
    T, D = tok.shape
    seg, width = q.shape
    hd = width // heads
    loads = [
        pltpu.make_async_copy(a, b, ws.at[n])
        for n, (a, b) in enumerate(
            ((w_in, wo.at[0]), (wg_in.at[0], wg), (wu_in.at[0], wu), (wd_in.at[0], wd))
        )
    ]
    for load in loads:
        load.start()

    def at_z(zz):
        return {"tp": 2 * lax.rem(zz + zn, zn) + c}

    def peer(d):
        return lax.rem(s + d, sp)

    def behind(d):
        return lax.rem(s + sp - d, sp)

    barrier = pltpu.get_barrier_semaphore()
    pl.semaphore_signal(barrier, inc=1, device_id={"tp": partner}, device_id_type=MESH)
    for i in range(1, zn):
        pl.semaphore_signal(barrier, inc=1, device_id=at_z(z + i), device_id_type=MESH)
    for d in range(1, sp):
        pl.semaphore_signal(barrier, inc=1, device_id={"sp": peer(d)}, device_id_type=MESH)
    pl.semaphore_wait(barrier, 1 + (zn - 1) + (sp - 1))

    pairs = ((k, ka), (v, va))
    square = sp == 4 and heads % 2 == 0 and (width // 2) % 128 == 0
    splits = 2 if square else 1
    lanes = width // splits

    def strip(f):
        return slice(f * lanes, (f + 1) * lanes)

    def share(n, f, d):
        src, dst = pairs[n]
        return rcopy(
            src.at[:, strip(f)], dst.at[d, :, strip(f)], ks.at[n, f, d], krs.at[n, f, d], {"sp": peer(d)}
        )

    def share_gate(d):
        return rcopy(g, ga.at[d], gs.at[0, d], gs.at[1, d], {"sp": peer(d)})

    def pass_kv(n, f, d, to, slot):
        dst = pairs[n][1]
        return rcopy(
            dst.at[d, :, strip(f)], dst.at[slot, :, strip(f)], kx.at[n, f], krs.at[n, f, slot],
            {"sp": lax.rem(to + sp, sp)},
        )

    def sends(d):
        if not square:
            return s + d < sp
        if d == 3:
            return s > sp
        return jnp.logical_and(s + d < sp, s != 1) if d == 1 else s + d < sp

    def relays(f, d):
        if not square:
            return ()
        corner = jnp.logical_and(s == 3, d == 2)
        last = (s == 1) if f == 0 else jnp.logical_and(s == 2, d == 2)
        return ((corner, s - 1, 1), (last, s + 2 - f, 3))

    def share_all(cond, f, d):
        @pl.when(cond)
        def _():
            for n in range(2):
                share(n, f, d).start()

    for d in range(1, sp):

        @pl.when(s + d < sp)
        def _():
            share_gate(d).start()

    for f in range(splits):
        for d in range(1, sp):
            if square and d == 2:
                share_all(s == 1, f, d)
                share_all(s == 0, 1 - f, d)
            else:
                share_all(sends(d), f, d)

    weights = rcopy(w_in, wo.at[1], wxs.at[0], wxs.at[1], {"tp": partner})
    weights.start()

    many = info.shape[2]
    here = lax.broadcasted_iota(jnp.int32, (many, T), 0)
    hit = jnp.zeros((many, T), F32)
    wt = jnp.zeros((many, T), F32)
    for r in range(ids.shape[0]):
        same = ids[r : r + 1, :] == here
        hit = hit + jnp.where(same, 1.0, 0.0)
        wt = wt + jnp.where(same, rw[r : r + 1, :], 0.0)
    before = lax.broadcasted_iota(jnp.int32, (T, T), 0) < lax.broadcasted_iota(jnp.int32, (T, T), 1)
    rank = jnp.dot(
        hit.astype(BF16), jnp.where(before, 1.0, 0.0).astype(BF16), preferred_element_type=F32
    )
    info[z, 0] = jnp.where(hit > 0.5, rank, -1.0)
    info[z, 1] = wt

    def aux(i, origin):
        return rcopy(info.at[origin], info.at[origin], as_.at[i], ars.at[i], at_z(z + i))

    for i in range(1, zn):
        aux(i, z).start()

    tile = math.gcd(seg, 256)
    log2e = 1.4426950408889634
    coef = hd ** (-0.5) * log2e
    units = [(h, i) for h in range(heads) for i in range(seg // tile)]
    each_split = heads // splits

    def scores(h, i, kb, gb):
        qt = q[i * tile : (i + 1) * tile, h * hd : (h + 1) * hd]
        return (
            lax.dot_general(qt, kb, (((1,), (1,)), ((), ())), preferred_element_type=F32) * coef
            - gb * log2e
        )

    for h, i in units:
        cols = slice(h * hd, (h + 1) * hd)
        seen = (i + 1) * tile
        sc = scores(h, i, k[0:seen, cols], g[h : h + 1, 0:seen])
        row = lax.broadcasted_iota(jnp.int32, sc.shape, 0) + i * tile
        col = lax.broadcasted_iota(jnp.int32, sc.shape, 1)
        sc = jnp.where(col <= row, sc, -1e30)
        peak = jnp.max(sc, axis=1, keepdims=True)
        ex = jnp.exp2(sc - peak)
        at = slice(i * tile, seen)
        top_s[h, at] = peak
        sum_s[h, at] = jnp.sum(ex, axis=1, keepdims=True)
        acc_s[h, at] = jnp.dot(ex.astype(BF16), v[0:seen, cols], preferred_element_type=F32)

    def land(f, d):
        for n in range(2):
            share(n, f, d).wait_recv()
            for cond, to, slot in relays(f, d):

                @pl.when(cond)
                def _():
                    pass_kv(n, f, d, to, slot).start()

    def absorb(f, d):
        for h, i in units:
            if h // each_split != f:
                continue
            cols = slice(h * hd, (h + 1) * hd)
            at = slice(i * tile, (i + 1) * tile)
            sc = scores(h, i, ka[d, :, cols], ga[d, h : h + 1, :])
            peak = top_s[h, at]
            new = jnp.maximum(peak, jnp.max(sc, axis=1, keepdims=True))
            ex = jnp.exp2(sc - new)
            fix = jnp.exp2(peak - new)
            top_s[h, at] = new
            sum_s[h, at] = sum_s[h, at] * fix + jnp.sum(ex, axis=1, keepdims=True)
            acc_s[h, at] = acc_s[h, at] * fix + jnp.dot(
                ex.astype(BF16), va[d, :, cols], preferred_element_type=F32
            )

    def step(i, _):
        if not square:
            share_gate(i).wait_recv()
            land(0, i)
            absorb(0, i)
            return 0
        d = jnp.where(i == 1, jnp.where(s == 1, 1, 2), jnp.where(i == 2, 1, 3))
        early = jnp.logical_and(s == 2, d == 2)
        share_gate(d).wait_recv()

        @pl.when(early)
        def _():
            land(1, d)

        land(0, d)
        absorb(0, d)

        @pl.when(jnp.logical_not(early))
        def _():
            land(1, d)

        absorb(1, d)
        return 0

    lax.fori_loop(1, s + 1, step, 0)
    for h, i in units:
        for b in range(i * tile // T, (i + 1) * tile // T):
            at = slice(b * T, (b + 1) * T)
            att[b % 2, b // 2, :, h * hd : (h + 1) * hd] = (acc_s[h, at] / sum_s[h, at]).astype(BF16)
    heads_swap = rcopy(att.at[1 - c], attp, hs.at[0], hs.at[1], {"tp": partner})
    heads_swap.start()
    loads[0].wait()
    weights.wait_recv()
    heads_swap.wait_recv()

    halves = 2
    part = D // halves
    chunk = math.gcd(part, 512)
    mine = att[c].reshape(zn * T, width)
    other = attp[...].reshape(zn * T, width)

    def hop(up, dest, h):
        cut = slice(h * part, (h + 1) * part)
        src, dst = (sup, rup) if up else (sdn, rdn)
        return rcopy(
            src.at[dest, :, cut], dst.at[dest, :, cut], us.at[up, dest, h], urs.at[up, dest, h],
            at_z(z + 1 if up else z - 1),
        )

    def project(h):
        for n in range(part // chunk):
            cut = slice(h * part + n * chunk, h * part + (n + 1) * chunk)
            got = jnp.dot(mine, wo[0, :, cut], preferred_element_type=F32) + jnp.dot(
                other, wo[1, :, cut], preferred_element_type=F32
            )
            pf[:, :, cut] = got.reshape(zn, T, chunk)

    def push(tau, h):
        cut = slice(h * part, (h + 1) * part)
        for up in (1, 0):
            wave = tau - z if up else tau - (zn - 1 - z)
            dest = zn - 1 - wave if up else wave
            going = jnp.logical_and(wave >= 0, z < dest if up else z > dest)
            first = z == 0 if up else z == zn - 1
            inner = z > 0 if up else z < zn - 1
            src, dst = (sup, rup) if up else (sdn, rdn)

            @pl.when(jnp.logical_and(going, first))
            def _():
                src[dest, :, cut] = pf[dest, :, cut].astype(BF16)
                hop(up, dest, h).start()

            @pl.when(jnp.logical_and(going, inner))
            def _():
                hop(up, dest, h).wait_recv()
                src[dest, :, cut] = (pf[dest, :, cut] + dst[dest, :, cut].astype(F32)).astype(BF16)
                hop(up, dest, h).start()

    for h in range(halves):
        project(h)
    for tau in range(zn - 1):
        for h in range(halves):
            push(tau, h)
    for h in range(halves):
        cut = slice(h * part, (h + 1) * part)

        @pl.when(z > 0)
        def _():
            hop(1, z, h).wait_recv()
            pf[z, :, cut] = pf[z, :, cut] + rup[z, :, cut].astype(F32)

        @pl.when(z < zn - 1)
        def _():
            hop(0, z, h).wait_recv()
            pf[z, :, cut] = pf[z, :, cut] + rdn[z, :, cut].astype(F32)

    st = (tok[...].astype(F32) + pf[z]).astype(BF16)
    out[...] = st
    wide = st.astype(F32)
    inverse = lax.rsqrt(jnp.mean(wide * wide, axis=1, keepdims=True) + 1e-05)
    ng[z] = (wide * inverse * gain[...]).astype(BF16)

    high = lax.div(2 * z, zn)
    low_z = z + high * (zn - 1 - 2 * z)

    def origin(j):
        if j == 0:
            return z
        a = (j + 1) // 2
        near = lax.div(zn + low_z - a, zn)
        o = near * (low_z + (a if j % 2 == 0 else -a)) + (1 - near) * j
        return o + high * (zn - 1 - 2 * o)

    def along(o):
        up = lax.div(zn + z - o - 1, zn)
        far = up * (z - o) + (1 - up) * (o - z)
        return up, far

    def carry(o, up, far):
        ref = ng.at[o]
        return rcopy(ref, ref, ns.at[up, far], nrs.at[up, far], at_z(z + 2 * up - 1))

    def arrived(o, up, far):
        ref = ng.at[o]
        return rcopy(ref, ref, ns.at[up, far], nrs.at[up, far - 1], at_z(z))

    def onward(o, up, far, act):
        goes = z + 2 * up - 1

        @pl.when(jnp.logical_and(goes >= 0, goes < zn))
        def _():
            act(carry(o, up, far))

    def own_block(act):
        @pl.when(z < zn - 1)
        def _():
            act(carry(z, 1, 0))

        @pl.when(z > 0)
        def _():
            act(carry(z, 0, 0))

    own_block(lambda cp: cp.start())

    def route(j, d):
        return rcopy(
            db.at[j, peer(d)], rows.at[j, s, c], ds_.at[j, d], drs.at[j, d], {"sp": peer(d)}
        )

    def routed(j, d):
        return rcopy(
            db.at[j, peer(d)], rows.at[j, behind(d), c], ds_.at[j, d], drs.at[j, d], {"sp": peer(d)}
        )

    def forward(j, d):
        ref = rows.at[j, behind(d), c]
        return rcopy(ref, ref, fs.at[j, d], frs.at[j, d], {"tp": partner})

    def forwarded(j, d):
        ref = rows.at[j, behind(d), 1 - c]
        return rcopy(ref, ref, fs.at[j, d], frs.at[j, d], {"tp": partner})

    def swap_out(j, d):
        return rcopy(y.at[j, peer(d), 1 - c], pr.at[j, d], ps.at[j, d], prs.at[j, d], {"tp": partner})

    def back(j, d, slot):
        return rcopy(cs.at[j, d], eb.at[j, slot], es.at[j, d], ers.at[j, d], {"sp": peer(d)})

    def reduce_out(j):
        return rcopy(mb.at[j], rr.at[z], ms.at[j], mrs.at[z], at_z(origin(j)))

    def reduced(i):
        zz = lax.rem(z + i, zn)
        return rcopy(mb.at[0], rr.at[zz], ms.at[0], mrs.at[zz], at_z(z))

    def dispatch(j):
        o = origin(j)
        if j > 0:
            up, far = along(o)
            arrived(o, up, far).wait_recv()
            onward(o, up, far, lambda cp: cp.start())
            aux(lax.rem(z - o + zn, zn), o).wait_recv()
        spots = lax.broadcasted_iota(jnp.int32, (cap, T), 0).astype(F32)
        for e in range(sp):
            code[e * cap : (e + 1) * cap] = jnp.where(info[o, 0, e : e + 1, :] == spots, 1.0, 0.0)
        moved = jnp.dot(code[...].astype(BF16), ng[o], preferred_element_type=F32)
        for e in range(sp):
            db[j, e] = moved[e * cap : (e + 1) * cap].astype(BF16)
        for d in range(1, sp):
            route(j, d).start()
        rows[j, s, c] = db[j, s]
        forward(j, 0).start()
        for e in range(sp):
            code[e * cap : (e + 1) * cap] = jnp.where(
                info[o, 0, e : e + 1, :] == spots, jnp.broadcast_to(info[o, 1, e : e + 1, :], (cap, T)), 0.0
            )
        given = code[...]
        coarse = given.astype(BF16)
        combs[j, 0] = coarse
        combs[j, 1] = (given - coarse.astype(F32)).astype(BF16)

    def pass_on(j):
        def arrive(d, _):
            routed(j, d).wait_recv()
            forward(j, d).start()
            return 0

        lax.fori_loop(1, sp, arrive, 0)

    def each(count, body):
        if count * rows.shape[1] <= 64:
            for n in range(count):
                body(n)
        else:
            lax.fori_loop(0, count, lambda n, _: (body(n), 0)[1], 0)

    def expert(j):
        def landed(d, _):
            forwarded(j, d).wait_recv()
            return 0

        lax.fori_loop(0, sp, landed, 0)
        x = rows.at[j]
        many = sp * 2 * cap
        units = wg.shape[1]
        step = 256

        def into(start, size):
            cut = pl.ds(start, size)
            xv = x[...].reshape(many, D)
            gate = jnp.dot(xv, wg[:, cut], preferred_element_type=F32)
            up = jnp.dot(xv, wu[:, cut], preferred_element_type=F32)
            hid[:, cut] = (gate / (1.0 + jnp.exp(-gate)) * up).astype(BF16)

        each(units // step, lambda n: into(pl.multiple_of(n * step, step), step))
        if units % step:
            into(units - units % step, units % step)
        chunk = math.gcd(D, 512)

        def down(n):
            cut = pl.ds(pl.multiple_of(n * chunk, chunk), chunk)
            got = jnp.dot(hid[...], wd[:, cut], preferred_element_type=F32).astype(BF16)
            y[j, :, :, :, cut] = got.reshape(sp, 2, cap, chunk)

        each(D // chunk, down)
        for d in list(range(1, sp)) + [0]:
            swap_out(j, d).start()

    def give_back(j):
        def both(d):
            swap_out(j, d).wait_recv()
            return (y[j, peer(d), c].astype(F32) + pr[j, d].astype(F32)).astype(BF16)

        def send(d, _):
            cs[j, d] = both(d)
            back(j, d, s).start()
            return 0

        lax.fori_loop(1, sp, send, 0)
        eb[j, s] = both(0)

    def mix(j):
        for d in range(1, sp):
            back(j, d, behind(d)).wait_recv()
        ev = eb[j].reshape(sp * cap, D)
        dims = (((0,), (0,)), ((), ()))
        return lax.dot_general(combs[j, 0], ev, dims, preferred_element_type=F32) + lax.dot_general(
            combs[j, 1], ev, dims, preferred_element_type=F32
        )

    dispatch(0)
    if zn > 1:
        dispatch(1)
    for load in loads[1:]:
        load.wait()
    for j in range(zn):
        pass_on(j)
        if j + 2 < zn:
            dispatch(j + 2)
        expert(j)
        if j >= 2:
            give_back(j)
    give_back(1)
    give_back(0)
    for j in list(range(2, zn)) + [1]:
        mb[j] = mix(j).astype(BF16)
        reduce_out(j).start()
    total = out[...].astype(F32) + mix(0)
    for i in range(1, zn):
        reduced(i).wait_recv()
        total = total + rr[lax.rem(z + i, zn)].astype(F32)
    out[...] = total.astype(BF16)

    for d in range(1, sp):

        @pl.when(sends(d))
        def _():
            for n in range(2):
                for f in range(splits):
                    share(n, f, d).wait_send()

        @pl.when(s + d < sp)
        def _():
            share_gate(d).wait_send()

    for f in range(splits):
        for cond, to, slot in ((s == 3, s - 1, 1), (s == (2 if f else 1), s + 2 - f, 3)) if square else ():

            @pl.when(cond)
            def _():
                for n in range(2):
                    pass_kv(n, f, 2, to, slot).wait_send()

    weights.wait_send()
    heads_swap.wait_send()
    own_block(lambda cp: cp.wait_send())
    for kk in range(zn - 1):
        for h in range(halves):
            for up in (1, 0):
                dest = zn - 1 - kk if up else kk

                @pl.when(z < dest if up else z > dest)
                def _():
                    hop(up, dest, h).wait_send()

    for j in range(zn):
        if j > 0:
            aux(j, z).wait_send()
            o = origin(j)
            onward(o, *along(o), lambda cp: cp.wait_send())
            reduce_out(j).wait_send()

        def drain(d, _):
            forward(j, d).wait_send()
            swap_out(j, d).wait_send()
            return 0

        lax.fori_loop(0, sp, drain, 0)
        for d in range(1, sp):
            route(j, d).wait_send()
            back(j, d, s).wait_send()


def shards(
    tokens,
    query_vectors,
    key_vectors,
    value_vectors,
    cum_gate,
    out_weight,
    norm_gain,
    gate_weight,
    up_weight,
    down_weight,
    expert_ids,
    route_weights,
):
    sp = lax.axis_size("sp")
    tp = lax.axis_size("tp")
    zn = tp // 2
    seg, width = query_vectors.shape
    heads = cum_gate.shape[1]
    T, D = tokens.shape
    dma = pltpu.SemaphoreType.DMA

    n_experts = gate_weight.shape[0] * sp
    top = expert_ids.shape[1]
    cap = max(2, 3 * T * top // (2 * n_experts))
    cap = -(-cap // 8) * 8
    slots = n_experts * cap
    kinds = -(-n_experts // 8) * 8
    fh = gate_weight.shape[2]

    def vm(*shape, kind=BF16):
        return pltpu.VMEM(shape, kind)

    return pl.pallas_call(
        functools.partial(layer_kernel, sp, zn, heads, cap),
        out_shape=jax.ShapeDtypeStruct((T, D), BF16),
        in_specs=vmem_specs(8) + [pl.BlockSpec(memory_space=pl.ANY)] * 4,
        out_specs=vmem_specs(1)[0],
        scratch_shapes=[
            vm(sp, seg, width), vm(sp, seg, width), vm(sp, heads, seg, kind=F32),
            vm(2, zn, T, width), vm(zn, T, width),
            vm(heads, seg, 1, kind=F32), vm(heads, seg, 1, kind=F32),
            vm(heads, seg, width // heads, kind=F32),
            vm(2, width, D), vm(zn, T, D, kind=F32),
            vm(zn, T, D), vm(zn, T, D), vm(zn, T, D), vm(zn, T, D), vm(zn, T, D),
            vm(zn, 2, kinds, T, kind=F32), vm(slots, T, kind=F32), vm(zn, 2, slots, T),
            vm(D, fh), vm(D, fh), vm(fh, D),
            vm(zn, sp, cap, D),
            vm(zn, sp, 2, cap, D),
            vm(sp * 2 * cap, fh),
            vm(zn, sp, 2, cap, D),
            vm(zn, sp, cap, D), vm(zn, sp, cap, D), vm(zn, sp, cap, D),
            vm(zn, T, D), vm(zn, T, D),
            dma((2, 2, sp)), dma((2, 2, sp)), dma((2, 2)), dma((2, sp)),
            dma((4,)), dma((2,)), dma((2,)),
            dma((zn,)), dma((zn,)),
            dma((2, zn, 2)), dma((2, zn, 2)),
            dma((2, zn)), dma((2, zn)),
            dma((zn, sp)), dma((zn, sp)),
            dma((zn, sp)), dma((zn, sp)),
            dma((zn, sp)), dma((zn, sp)),
            dma((zn, sp)), dma((zn, sp)),
            dma((zn,)), dma((zn,)),
        ],
        compiler_params=pltpu.CompilerParams(
            collective_id=0, has_side_effects=True, vmem_limit_bytes=VMEM_LIMIT
        ),
        name="layer",
    )(
        query_vectors, key_vectors, value_vectors, cum_gate.T, tokens, norm_gain[None, :],
        expert_ids.T, route_weights.T, out_weight, gate_weight, up_weight, down_weight,
    )


def solution(mesh):
    in_specs = (
        P(("sp", "tp"), None),
        P("sp", "tp"),
        P("sp", "tp"),
        P("sp", "tp"),
        P("sp", "tp"),
        P("tp", None),
        P(),
        P("sp", None, "tp"),
        P("sp", None, "tp"),
        P("sp", "tp", None),
        P(("sp", "tp"), None),
        P(("sp", "tp"), None),
    )
    out_specs = P(("sp", "tp"), None)
    return jax.shard_map(shards, mesh=mesh, in_specs=in_specs, out_specs=out_specs, check_vma=False)
```

```python
import functools
import math

import jax
import jax.numpy as jnp
from jax import lax
from jax.experimental import pallas as pl
from jax.experimental.pallas import tpu as pltpu
from jax.sharding import PartitionSpec as P

MESH = pl.DeviceIdType.MESH
VMEM_LIMIT = 60 * 1024 * 1024
F32 = jnp.float32
BF16 = jnp.bfloat16


def rcopy(src, dst, ssem, rsem, where):
    return pltpu.make_async_remote_copy(
        src_ref=src, dst_ref=dst, send_sem=ssem, recv_sem=rsem, device_id=where, device_id_type=MESH
    )


def vmem_specs(count):
    return [pl.BlockSpec(memory_space=pltpu.VMEM)] * count


def layer_kernel(
    sp, zn, heads, cap,
    q, k, v, g, tok, gain, ids, rw, w_in, wg_in, wu_in, wd_in, out,
    ka, va, ga, att, attp, top_s, sum_s, acc_s, wo, pf, sup, sdn, rup, rdn, ng,
    info, code, combs, wg, wu, wd, db, rows, hid, y, pr, cs, eb, mb, rr, bs, zb,
    ks, krs, kx, gs, ws, wxs, hs, as_, ars, us, urs, ns, nrs, ds_, drs, fs, frs, ps, prs, es, ers, ms, mrs, ffs, ffrs, zs, zrs, bfs, bfrs,
):
    s, t = lax.axis_index("sp"), lax.axis_index("tp")
    z, c = lax.div(t, 2), lax.rem(t, 2)
    partner = t + 1 - 2 * c
    T, D = tok.shape
    seg, width = q.shape
    hd = width // heads
    loads = [
        pltpu.make_async_copy(a, b, ws.at[n])
        for n, (a, b) in enumerate(
            ((w_in, wo.at[0]), (wg_in.at[0], wg), (wu_in.at[0], wu), (wd_in.at[0], wd))
        )
    ]
    for load in loads:
        load.start()

    def at_z(zz):
        return {"tp": 2 * lax.rem(zz + zn, zn) + c}

    def ahead(d):
        return lax.rem(s + d, sp)

    bits = max(sp - 1, 1).bit_length()
    paired = sp == 1 << bits

    def peer(d):
        if not paired:
            return lax.rem(s + d, sp)
        return sum(lax.rem(lax.div(s, 1 << b) + d // (1 << b), 2) * (1 << b) for b in range(bits))

    def behind(d):
        return peer(d) if paired else lax.rem(s + sp - d, sp)

    barrier = pltpu.get_barrier_semaphore()
    pl.semaphore_signal(barrier, inc=1, device_id={"tp": partner}, device_id_type=MESH)
    for i in range(1, zn):
        pl.semaphore_signal(barrier, inc=1, device_id=at_z(z + i), device_id_type=MESH)
    for d in range(1, sp):
        pl.semaphore_signal(barrier, inc=1, device_id={"sp": ahead(d)}, device_id_type=MESH)
    pl.semaphore_wait(barrier, 1 + (zn - 1) + (sp - 1))

    pairs = ((k, ka), (v, va))
    square = sp == 4 and heads % 2 == 0 and (width // 2) % 128 == 0
    splits = 2 if square else 1
    lanes = width // splits

    def strip(f):
        return slice(f * lanes, (f + 1) * lanes)

    def share(n, f, d):
        src, dst = pairs[n]
        return rcopy(
            src.at[:, strip(f)], dst.at[d, :, strip(f)], ks.at[n, f, d], krs.at[n, f, d], {"sp": ahead(d)}
        )

    def share_gate(d):
        return rcopy(g, ga.at[d], gs.at[0, d], gs.at[1, d], {"sp": ahead(d)})

    def pass_kv(n, f, d, to, slot):
        dst = pairs[n][1]
        return rcopy(
            dst.at[d, :, strip(f)], dst.at[slot, :, strip(f)], kx.at[n, f], krs.at[n, f, slot],
            {"sp": lax.rem(to + sp, sp)},
        )

    def sends(d):
        if not square:
            return s + d < sp
        if d == 3:
            return s > sp
        return jnp.logical_and(s + d < sp, s != 1) if d == 1 else s + d < sp

    def relays(f, d):
        if not square:
            return ()
        corner = jnp.logical_and(s == 3, d == 2)
        last = (s == 1) if f == 0 else jnp.logical_and(s == 2, d == 2)
        return ((corner, s - 1, 1), (last, s + 2 - f, 3))

    def share_all(cond, f, d):
        @pl.when(cond)
        def _():
            for n in range(2):
                share(n, f, d).start()

    for d in range(1, sp):

        @pl.when(s + d < sp)
        def _():
            share_gate(d).start()

    for f in range(splits):
        for d in range(1, sp):
            if square and d == 2:
                share_all(s == 1, f, d)
                share_all(s == 0, 1 - f, d)
            else:
                share_all(sends(d), f, d)

    weights = rcopy(w_in, wo.at[1], wxs.at[0], wxs.at[1], {"tp": partner})
    weights.start()

    many = info.shape[2]
    here = lax.broadcasted_iota(jnp.int32, (many, T), 0)
    hit = jnp.zeros((many, T), F32)
    wt = jnp.zeros((many, T), F32)
    for r in range(ids.shape[0]):
        same = ids[r : r + 1, :] == here
        hit = hit + jnp.where(same, 1.0, 0.0)
        wt = wt + jnp.where(same, rw[r : r + 1, :], 0.0)
    before = lax.broadcasted_iota(jnp.int32, (T, T), 0) < lax.broadcasted_iota(jnp.int32, (T, T), 1)
    rank = jnp.dot(
        hit.astype(BF16), jnp.where(before, 1.0, 0.0).astype(BF16), preferred_element_type=F32
    )
    info[z, 0] = jnp.where(hit > 0.5, rank, -1.0)
    info[z, 1] = wt

    def aux(i, origin):
        return rcopy(info.at[origin], info.at[origin], as_.at[i], ars.at[i], at_z(z + i))

    for i in range(1, zn):
        aux(i, z).start()

    tile = math.gcd(seg, 256)
    log2e = 1.4426950408889634
    coef = hd ** (-0.5) * log2e
    units = [(h, i) for h in range(heads) for i in range(seg // tile)]
    each_split = heads // splits

    def scores(h, i, kb, gb):
        qt = q[i * tile : (i + 1) * tile, h * hd : (h + 1) * hd]
        return (
            lax.dot_general(qt, kb, (((1,), (1,)), ((), ())), preferred_element_type=F32) * coef
            - gb * log2e
        )

    for h, i in units:
        cols = slice(h * hd, (h + 1) * hd)
        seen = (i + 1) * tile
        sc = scores(h, i, k[0:seen, cols], g[h : h + 1, 0:seen])
        row = lax.broadcasted_iota(jnp.int32, sc.shape, 0) + i * tile
        col = lax.broadcasted_iota(jnp.int32, sc.shape, 1)
        sc = jnp.where(col <= row, sc, -1e30)
        peak = jnp.max(sc, axis=1, keepdims=True)
        ex = jnp.exp2(sc - peak)
        at = slice(i * tile, seen)
        top_s[h, at] = peak
        sum_s[h, at] = jnp.sum(ex, axis=1, keepdims=True)
        acc_s[h, at] = jnp.dot(ex.astype(BF16), v[0:seen, cols], preferred_element_type=F32)

    def land(f, d):
        for n in range(2):
            share(n, f, d).wait_recv()
            for cond, to, slot in relays(f, d):

                @pl.when(cond)
                def _():
                    pass_kv(n, f, d, to, slot).start()

    def absorb(f, d):
        for h, i in units:
            if h // each_split != f:
                continue
            cols = slice(h * hd, (h + 1) * hd)
            at = slice(i * tile, (i + 1) * tile)
            sc = scores(h, i, ka[d, :, cols], ga[d, h : h + 1, :])
            peak = top_s[h, at]
            new = jnp.maximum(peak, jnp.max(sc, axis=1, keepdims=True))
            ex = jnp.exp2(sc - new)
            fix = jnp.exp2(peak - new)
            top_s[h, at] = new
            sum_s[h, at] = sum_s[h, at] * fix + jnp.sum(ex, axis=1, keepdims=True)
            acc_s[h, at] = acc_s[h, at] * fix + jnp.dot(
                ex.astype(BF16), va[d, :, cols], preferred_element_type=F32
            )

    def step(i, _):
        if not square:
            share_gate(i).wait_recv()
            land(0, i)
            absorb(0, i)
            return 0
        d = jnp.where(i == 1, jnp.where(s == 1, 1, 2), jnp.where(i == 2, 1, 3))
        early = jnp.logical_and(s == 2, d == 2)
        share_gate(d).wait_recv()

        @pl.when(early)
        def _():
            land(1, d)

        land(0, d)
        absorb(0, d)

        @pl.when(jnp.logical_not(early))
        def _():
            land(1, d)

        absorb(1, d)
        return 0

    lax.fori_loop(1, s + 1, step, 0)
    for h, i in units:
        for b in range(i * tile // T, (i + 1) * tile // T):
            at = slice(b * T, (b + 1) * T)
            att[b % 2, b // 2, :, h * hd : (h + 1) * hd] = (acc_s[h, at] / sum_s[h, at]).astype(BF16)
    heads_swap = rcopy(att.at[1 - c], attp, hs.at[0], hs.at[1], {"tp": partner})
    heads_swap.start()
    loads[0].wait()
    weights.wait_recv()
    heads_swap.wait_recv()

    halves = 2
    part = D // halves
    chunk = math.gcd(part, 512)
    mine = att[c].reshape(zn * T, width)
    other = attp[...].reshape(zn * T, width)

    def hop(up, dest, h):
        cut = slice(h * part, (h + 1) * part)
        src, dst = (sup, rup) if up else (sdn, rdn)
        return rcopy(
            src.at[dest, :, cut], dst.at[dest, :, cut], us.at[up, dest, h], urs.at[up, dest, h],
            at_z(z + 1 if up else z - 1),
        )

    def project(h):
        for n in range(part // chunk):
            cut = slice(h * part + n * chunk, h * part + (n + 1) * chunk)
            got = jnp.dot(mine, wo[0, :, cut], preferred_element_type=F32) + jnp.dot(
                other, wo[1, :, cut], preferred_element_type=F32
            )
            pf[:, :, cut] = got.reshape(zn, T, chunk)

    def push(tau, h):
        cut = slice(h * part, (h + 1) * part)
        for up in (1, 0):
            wave = tau - z if up else tau - (zn - 1 - z)
            dest = zn - 1 - wave if up else wave
            going = jnp.logical_and(wave >= 0, z < dest if up else z > dest)
            first = z == 0 if up else z == zn - 1
            inner = z > 0 if up else z < zn - 1
            src, dst = (sup, rup) if up else (sdn, rdn)

            @pl.when(jnp.logical_and(going, first))
            def _():
                src[dest, :, cut] = pf[dest, :, cut].astype(BF16)
                hop(up, dest, h).start()

            @pl.when(jnp.logical_and(going, inner))
            def _():
                hop(up, dest, h).wait_recv()
                src[dest, :, cut] = (pf[dest, :, cut] + dst[dest, :, cut].astype(F32)).astype(BF16)
                hop(up, dest, h).start()

    for h in range(halves):
        project(h)
    for tau in range(zn - 1):
        for h in range(halves):
            push(tau, h)
    for h in range(halves):
        cut = slice(h * part, (h + 1) * part)

        @pl.when(z > 0)
        def _():
            hop(1, z, h).wait_recv()
            pf[z, :, cut] = pf[z, :, cut] + rup[z, :, cut].astype(F32)

        @pl.when(z < zn - 1)
        def _():
            hop(0, z, h).wait_recv()
            pf[z, :, cut] = pf[z, :, cut] + rdn[z, :, cut].astype(F32)

    st = (tok[...].astype(F32) + pf[z]).astype(BF16)
    out[...] = st
    wide = st.astype(F32)
    inverse = lax.rsqrt(jnp.mean(wide * wide, axis=1, keepdims=True) + 1e-05)
    ng[z] = (wide * inverse * gain[...]).astype(BF16)

    high = lax.div(2 * z, zn)
    low_z = z + high * (zn - 1 - 2 * z)

    def origin(j):
        if j == 0:
            return z
        a = (j + 1) // 2
        near = lax.div(zn + low_z - a, zn)
        o = near * (low_z + (a if j % 2 == 0 else -a)) + (1 - near) * j
        return o + high * (zn - 1 - 2 * o)

    def along(o):
        up = lax.div(zn + z - o - 1, zn)
        far = up * (z - o) + (1 - up) * (o - z)
        return up, far

    in_z, out_z = D // 4, bs.shape[3]
    first_in, rest_in = slice(0, in_z), slice(in_z, D)
    first_out, rest_out = slice(0, out_z), slice(out_z, D)

    def block(kind, o):
        return rows.at[o, :, c, :, first_in] if kind else ng.at[o, :, rest_in]

    def carry(kind, o, up, far):
        ref = block(kind, o)
        return rcopy(ref, ref, ns.at[kind, up, far], nrs.at[kind, up, far], at_z(z + 2 * up - 1))

    def arrived(kind, o, up, far):
        ref = block(kind, o)
        return rcopy(ref, ref, ns.at[kind, up, far], nrs.at[kind, up, far - 1], at_z(z))

    def onward(kind, o, up, far, act):
        goes = z + 2 * up - 1

        @pl.when(jnp.logical_and(goes >= 0, goes < zn))
        def _():
            act(carry(kind, o, up, far))

    def own_block(kind, act):
        @pl.when(z < zn - 1)
        def _():
            act(carry(kind, z, 1, 0))

        @pl.when(z > 0)
        def _():
            act(carry(kind, z, 0, 0))

    own_block(0, lambda cp: cp.start())

    def span(j):
        return rest_in if j > 0 else slice(0, D)

    def route(j, d):
        return rcopy(
            db.at[j, peer(d), :, span(j)], rows.at[origin(j), s, c, :, span(j)],
            ds_.at[j, d], drs.at[j, d], {"sp": peer(d)},
        )

    def routed(j, d):
        return rcopy(
            db.at[j, peer(d), :, span(j)], rows.at[origin(j), behind(d), c, :, span(j)],
            ds_.at[j, d], drs.at[j, d], {"sp": peer(d)},
        )

    def forward(j, d):
        ref = rows.at[origin(j), behind(d), c, :, span(j)]
        return rcopy(ref, ref, fs.at[j, d], frs.at[j, d], {"tp": partner})

    def forwarded(j, d):
        ref = rows.at[origin(j), behind(d), 1 - c, :, span(j)]
        return rcopy(ref, ref, fs.at[j, d], frs.at[j, d], {"tp": partner})

    def forward_first(j, core):
        ref = rows.at[origin(j), :, core, :, first_in]
        return rcopy(ref, ref, ffs.at[j], ffrs.at[j], {"tp": partner})

    def swap_out(j, d):
        return rcopy(y.at[j, peer(d), 1 - c], pr.at[j, d], ps.at[j, d], prs.at[j, d], {"tp": partner})

    def back(j, d, slot):
        return rcopy(
            cs.at[j, d, :, rest_out], eb.at[j, slot, :, rest_out], es.at[j, d], ers.at[j, d],
            {"sp": peer(d)},
        )

    def back_first(d, slot):
        return rcopy(
            cs.at[0, d, :, first_out], eb.at[0, slot, :, first_out], bfs.at[d], bfrs.at[d],
            {"sp": peer(d)},
        )

    def home(j):
        return rcopy(bs.at[j], zb.at[z], zs.at[j], zrs.at[z], at_z(origin(j)))

    def homed(zz):
        return rcopy(bs.at[0], zb.at[zz], zs.at[0], zrs.at[zz], at_z(z))

    def reduce_out(j):
        return rcopy(
            mb.at[j, :, rest_out], rr.at[z, :, rest_out], ms.at[j], mrs.at[z], at_z(origin(j))
        )

    def reduced(i):
        zz = lax.rem(z + i, zn)
        return rcopy(mb.at[0, :, rest_out], rr.at[zz, :, rest_out], ms.at[0], mrs.at[zz], at_z(z))

    def relay(kind, j):
        o = origin(j)
        up, far = along(o)

        def act(cp):
            arrived(kind, o, up, far).wait_recv()
            cp.start()

        onward(kind, o, up, far, act)

    def ended(kind, j):
        o = origin(j)
        up, far = along(o)
        goes = z + 2 * up - 1

        @pl.when(jnp.logical_or(goes < 0, goes >= zn))
        def _():
            arrived(kind, o, up, far).wait_recv()

    def dispatch(j):
        o = origin(j)
        if j > 0:
            ended(0, j)
            aux(lax.rem(z - o + zn, zn), o).wait_recv()
        spots = lax.broadcasted_iota(jnp.int32, (cap, T), 0).astype(F32)
        for e in range(sp):
            code[e * cap : (e + 1) * cap] = jnp.where(info[o, 0, e : e + 1, :] == spots, 1.0, 0.0)
        moved = jnp.dot(code[...].astype(BF16), ng[o, :, span(j)], preferred_element_type=F32)
        for e in range(sp):
            db[j, e, :, span(j)] = moved[e * cap : (e + 1) * cap].astype(BF16)
        for d in range(sp - 1, 0, -1):
            route(j, d).start()
        rows[o, s, c, :, span(j)] = db[j, s, :, span(j)]
        forward(j, 0).start()
        for e in range(sp):
            code[e * cap : (e + 1) * cap] = jnp.where(
                info[o, 0, e : e + 1, :] == spots, jnp.broadcast_to(info[o, 1, e : e + 1, :], (cap, T)), 0.0
            )
        given = code[...]
        coarse = given.astype(BF16)
        combs[j, 0] = coarse
        combs[j, 1] = (given - coarse.astype(F32)).astype(BF16)

    def pass_on(j):
        def arrive(d, _):
            routed(j, d).wait_recv()
            forward(j, d).start()
            return 0

        lax.fori_loop(1, sp, arrive, 0)

    def pass_first(j):
        ended(1, j)
        forward_first(j, c).start()

    def each(count, body):
        if count * rows.shape[1] <= 64:
            for n in range(count):
                body(n)
        else:
            lax.fori_loop(0, count, lambda n, _: (body(n), 0)[1], 0)

    def expert(j):
        def landed(d, _):
            forwarded(j, d).wait_recv()
            return 0

        lax.fori_loop(0, sp, landed, 0)
        if j > 0:
            forward_first(j, 1 - c).wait_recv()
        x = rows.at[origin(j)]
        many = sp * 2 * cap
        units = wg.shape[1]
        step = 256

        def into(start, size):
            cut = pl.ds(start, size)
            xv = x[...].reshape(many, D)
            gate = jnp.dot(xv, wg[:, cut], preferred_element_type=F32)
            up = jnp.dot(xv, wu[:, cut], preferred_element_type=F32)
            hid[:, cut] = (gate / (1.0 + jnp.exp(-gate)) * up).astype(BF16)

        each(units // step, lambda n: into(pl.multiple_of(n * step, step), step))
        if units % step:
            into(units - units % step, units % step)
        chunk = math.gcd(D, 512)

        def down(n):
            cut = pl.ds(pl.multiple_of(n * chunk, chunk), chunk)
            got = jnp.dot(hid[...], wd[:, cut], preferred_element_type=F32).astype(BF16)
            y[j, :, :, :, cut] = got.reshape(sp, 2, cap, chunk)

        each(D // chunk, down)
        for d in range(sp - 1, -1, -1):
            swap_out(j, d).start()

    def give_back(j):
        def settle(d, ref):
            swap_out(j, d).wait_recv()
            got = y[j, peer(d), c].astype(F32) + pr[j, d].astype(F32)
            ref[:, rest_out] = got[:, rest_out].astype(BF16)
            if j > 0:
                bs[j, d] = got[:, first_out].astype(BF16)

        def send(n, _):
            d = sp - n
            settle(d, cs.at[j, d])
            back(j, d, s).start()
            return 0

        lax.fori_loop(1, sp, send, 0)
        settle(0, eb.at[j, s])
        if j > 0:
            home(j).start()

    def give_first():
        for i in range(1, zn):
            homed(lax.rem(z + i, zn)).wait_recv()

        def gather(d):
            got = y[0, peer(d), c, :, first_out].astype(F32) + pr[0, d, :, first_out].astype(F32)
            for i in range(1, zn):
                got = got + zb[lax.rem(z + i, zn), d].astype(F32)
            return got.astype(BF16)

        def send(n, _):
            d = sp - n
            cs[0, d, :, first_out] = gather(d)
            back_first(d, s).start()
            return 0

        lax.fori_loop(1, sp, send, 0)
        eb[0, s, :, first_out] = gather(0)

    def mix(j, cut):
        ev = eb[j, :, :, cut].reshape(sp * cap, cut.stop - cut.start)
        dims = (((0,), (0,)), ((), ()))
        return lax.dot_general(combs[j, 0], ev, dims, preferred_element_type=F32) + lax.dot_general(
            combs[j, 1], ev, dims, preferred_element_type=F32
        )

    def returned(j):
        for d in range(sp - 1, 0, -1):
            back(j, d, behind(d)).wait_recv()

    def mix_out(j):
        returned(j)
        mb[j, :, rest_out] = mix(j, rest_out).astype(BF16)
        reduce_out(j).start()

    dispatch(0)
    relay(0, 1)
    relay(0, 2)
    dispatch(1)
    for load in loads[1:]:
        load.wait()
    for j in range(zn):
        pass_on(j)
        if j == 0:
            dispatch(2)
            for n in range(3, zn):
                relay(0, n)
            own_block(1, lambda cp: cp.start())
        elif j + 2 < zn:
            dispatch(j + 2)
        if j > 0:
            if j == 1:
                relay(1, 1)
            if j + 1 < zn:
                relay(1, j + 1)
            pass_first(j)
        expert(j)
        if j > 0:
            give_back(j)
    give_back(0)
    for j in range(1, zn):
        mix_out(j)
    give_first()
    returned(0)
    total = out[:, rest_out].astype(F32) + mix(0, rest_out)
    for i in range(1, zn):
        reduced(i).wait_recv()
        total = total + rr[lax.rem(z + i, zn), :, rest_out].astype(F32)
    out[:, rest_out] = total.astype(BF16)
    for d in range(1, sp):
        back_first(d, behind(d)).wait_recv()
    out[:, first_out] = (out[:, first_out].astype(F32) + mix(0, first_out)).astype(BF16)

    for d in range(1, sp):

        @pl.when(sends(d))
        def _():
            for n in range(2):
                for f in range(splits):
                    share(n, f, d).wait_send()

        @pl.when(s + d < sp)
        def _():
            share_gate(d).wait_send()

    for f in range(splits):
        for cond, to, slot in ((s == 3, s - 1, 1), (s == (2 if f else 1), s + 2 - f, 3)) if square else ():

            @pl.when(cond)
            def _():
                for n in range(2):
                    pass_kv(n, f, 2, to, slot).wait_send()

    weights.wait_send()
    heads_swap.wait_send()
    for kind in (0, 1):
        own_block(kind, lambda cp: cp.wait_send())
    for kk in range(zn - 1):
        for h in range(halves):
            for up in (1, 0):
                dest = zn - 1 - kk if up else kk

                @pl.when(z < dest if up else z > dest)
                def _():
                    hop(up, dest, h).wait_send()

    for j in range(zn):
        if j > 0:
            aux(j, z).wait_send()
            o = origin(j)
            for kind in (0, 1):
                onward(kind, o, *along(o), lambda cp: cp.wait_send())
            reduce_out(j).wait_send()
            home(j).wait_send()
            forward_first(j, c).wait_send()

        def drain(d, _):
            forward(j, d).wait_send()
            swap_out(j, d).wait_send()
            return 0

        lax.fori_loop(0, sp, drain, 0)
        for d in range(1, sp):
            route(j, d).wait_send()
            back(j, d, s).wait_send()
            if j == 0:
                back_first(d, s).wait_send()


def shards(
    tokens,
    query_vectors,
    key_vectors,
    value_vectors,
    cum_gate,
    out_weight,
    norm_gain,
    gate_weight,
    up_weight,
    down_weight,
    expert_ids,
    route_weights,
):
    sp = lax.axis_size("sp")
    tp = lax.axis_size("tp")
    zn = tp // 2
    seg, width = query_vectors.shape
    heads = cum_gate.shape[1]
    T, D = tokens.shape
    dma = pltpu.SemaphoreType.DMA

    n_experts = gate_weight.shape[0] * sp
    top = expert_ids.shape[1]
    cap = max(2, 3 * T * top // (2 * n_experts))
    cap = -(-cap // 8) * 8
    slots = n_experts * cap
    kinds = -(-n_experts // 8) * 8
    fh = gate_weight.shape[2]

    def vm(*shape, kind=BF16):
        return pltpu.VMEM(shape, kind)

    return pl.pallas_call(
        functools.partial(layer_kernel, sp, zn, heads, cap),
        out_shape=jax.ShapeDtypeStruct((T, D), BF16),
        in_specs=vmem_specs(8) + [pl.BlockSpec(memory_space=pl.ANY)] * 4,
        out_specs=vmem_specs(1)[0],
        scratch_shapes=[
            vm(sp, seg, width), vm(sp, seg, width), vm(sp, heads, seg, kind=F32),
            vm(2, zn, T, width), vm(zn, T, width),
            vm(heads, seg, 1, kind=F32), vm(heads, seg, 1, kind=F32),
            vm(heads, seg, width // heads, kind=F32),
            vm(2, width, D), vm(zn, T, D, kind=F32),
            vm(zn, T, D), vm(zn, T, D), vm(zn, T, D), vm(zn, T, D), vm(zn, T, D),
            vm(zn, 2, kinds, T, kind=F32), vm(slots, T, kind=F32), vm(zn, 2, slots, T),
            vm(D, fh), vm(D, fh), vm(fh, D),
            vm(zn, sp, cap, D),
            vm(zn, sp, 2, cap, D),
            vm(sp * 2 * cap, fh),
            vm(zn, sp, 2, cap, D),
            vm(zn, sp, cap, D), vm(zn, sp, cap, D), vm(zn, sp, cap, D),
            vm(zn, T, D), vm(zn, T, D),
            vm(zn, sp, cap, D // 8), vm(zn, sp, cap, D // 8),
            dma((2, 2, sp)), dma((2, 2, sp)), dma((2, 2)), dma((2, sp)),
            dma((4,)), dma((2,)), dma((2,)),
            dma((zn,)), dma((zn,)),
            dma((2, zn, 2)), dma((2, zn, 2)),
            dma((2, 2, zn)), dma((2, 2, zn)),
            dma((zn, sp)), dma((zn, sp)),
            dma((zn, sp)), dma((zn, sp)),
            dma((zn, sp)), dma((zn, sp)),
            dma((zn, sp)), dma((zn, sp)),
            dma((zn,)), dma((zn,)),
            dma((zn,)), dma((zn,)), dma((zn,)), dma((zn,)),
            dma((sp,)), dma((sp,)),
        ],
        compiler_params=pltpu.CompilerParams(
            collective_id=0, has_side_effects=True, vmem_limit_bytes=VMEM_LIMIT
        ),
        name="layer",
    )(
        query_vectors, key_vectors, value_vectors, cum_gate.T, tokens, norm_gain[None, :],
        expert_ids.T, route_weights.T, out_weight, gate_weight, up_weight, down_weight,
    )


def solution(mesh):
    in_specs = (
        P(("sp", "tp"), None),
        P("sp", "tp"),
        P("sp", "tp"),
        P("sp", "tp"),
        P("sp", "tp"),
        P("tp", None),
        P(),
        P("sp", None, "tp"),
        P("sp", None, "tp"),
        P("sp", "tp", None),
        P(("sp", "tp"), None),
        P(("sp", "tp"), None),
    )
    out_specs = P(("sp", "tp"), None)
    return jax.shard_map(shards, mesh=mesh, in_specs=in_specs, out_specs=out_specs, check_vma=False)
```
